32 devices in a mesh: grp: 1, ep: 32 (over z, y, x, core).
Axes of the slice: x: 2, y: 2, z: 4, core: 2. Of those that a mesh axis runs over, the one named last changes fastest.
Arguments:
- tokens: bfloat16 [64, 2048], P('grp', 'ep'), may hold values from -6 to 6
- w_query: bfloat16 [2048, 1024], P('ep'), may hold values from -0.125 to 0.125
- w_key: bfloat16 [2048, 1024], P('ep'), may hold values from -0.125 to 0.125
- w_value: bfloat16 [2048, 1024], P('ep'), may hold values from -0.125 to 0.125
- w_forget: bfloat16 [2048, 16], P('ep'), may hold values from -0.125 to 0.125
- forget_bias: float32 [16], replicated, may hold values from -1 to 2
- cache_keys: bfloat16 [64, 1024, 1024], P(('grp', 'ep'))
- cache_values: bfloat16 [64, 1024, 1024], P(('grp', 'ep')), may hold values from -6 to 6
- cache_gates: float32 [64, 1024, 16], P(('grp', 'ep')), as said below
- lengths: int32 [64], P(('grp', 'ep')), may hold values from 128 to 1024, as said below
- w_out: bfloat16 [1024, 2048], P('ep'), may hold values from -0.1875 to 0.1875
- norm_gain: bfloat16 [2048], replicated, may hold values from 0.099609375 to 1.8984375
- w_router: bfloat16 [2048, 4], replicated, may hold values from -0.125 to 0.125
- routes: int32 [64, 2], P('grp'), may hold values from 0 to 3, all different within a row
- dense_gate: bfloat16 [2048], replicated, may hold values from -0.25 to 0.25
- dense_w_gate: bfloat16 [2048, 8192], P(None, 'ep'), may hold values from -0.125 to 0.125
- dense_w_up: bfloat16 [2048, 8192], P(None, 'ep'), may hold values from -0.125 to 0.125
- dense_w_down: bfloat16 [8192, 2048], P('ep'), may hold values from -0.125 to 0.125
- expert_w_gate: bfloat16 [2048, 16384], P(None, 'ep'), may hold values from -0.125 to 0.125
- expert_w_up: bfloat16 [2048, 16384], P(None, 'ep'), may hold values from -0.125 to 0.125
- expert_w_down: bfloat16 [16384, 2048], P('ep'), may hold values from -0.1875 to 0.1875
- final_gain: bfloat16 [2048], P('ep'), may hold values from 0.099609375 to 1.8984375
Outputs:
- result: bfloat16 [64, 2048], P('grp', 'ep')
The draws below stay inside these ranges and needn't reach their ends.
Inputs may be any that keep to these rules, and one draw needn't show every extreme that they name: `routes`: each row names 2 different experts; every expert is named by some row. `lengths`: the first sequence of each part holds 1024 positions. `cache_gates`: never rising along positions.
All inputs are finite; a program needn't handle non-finite values.
Results may differ from the reference program's by a relative error of at most 0.0085.
Values may be sent and summed in bfloat16 or wider, within the bound.
A program may use at most 128 MiB of HBM per device.

```python
import jax
import jax.numpy as jnp
from jax import lax

D = 2048
QUERY_GROUPS = 16
ATT = 1024
BATCH_LENGTH = 64
STORED_PLACES = 1024
EXPERT_FF = 4096
EXPERTS = 4
TOPK = 2
DENSE_FF = 8192


def draw_lengths(key, part):
    picked = jax.random.randint(jax.random.fold_in(key, 11), (BATCH_LENGTH,), STORED_PLACES // 8, STORED_PLACES + 1)
    return picked.at[0].set(STORED_PLACES).astype(jnp.int32)


def draw_cache_keys(key, part):
    base = jax.random.normal(jax.random.fold_in(key, 21), (BATCH_LENGTH, STORED_PLACES, ATT), jnp.float32)
    return base.astype(jnp.bfloat16)


def draw_cache_gates(key, part):
    lookup_matrix = jax.random.split(jax.random.fold_in(key, 31), 7)
    slow_share = 0.5
    lagging_portion = jax.random.uniform(lookup_matrix[0], (QUERY_GROUPS,), jnp.float32) < slow_share
    seq_factor = jnp.exp(jax.random.uniform(lookup_matrix[1], (BATCH_LENGTH, 1, 1), jnp.float32, -0.7, 0.7))
    pos_factor = jax.random.uniform(lookup_matrix[2], (BATCH_LENGTH, STORED_PLACES, 1), jnp.float32, 0.5, 1.5)
    slow_rate = jax.random.uniform(lookup_matrix[3], (BATCH_LENGTH, 1, QUERY_GROUPS), jnp.float32, 0.5, 2.0) / STORED_PLACES
    fast_rate = jax.random.uniform(lookup_matrix[4], (BATCH_LENGTH, 1, QUERY_GROUPS), jnp.float32, 1.0 / 100.0, 1.0 / 30.0)
    fading_speed = jnp.where(lagging_portion[None, None, :], slow_rate, fast_rate) * seq_factor * pos_factor
    spike_quantity = jax.random.uniform(lookup_matrix[5], (BATCH_LENGTH, STORED_PLACES, QUERY_GROUPS), jnp.float32) < 3.0 / STORED_PLACES
    shrink_multiplier = jnp.log(jax.random.uniform(lookup_matrix[6], (BATCH_LENGTH, STORED_PLACES, QUERY_GROUPS), jnp.float32, 0.5, 0.8))
    forget_each_token = -fading_speed + jnp.where(jnp.logical_and(spike_quantity, lagging_portion[None, None, :]), shrink_multiplier, 0.0)
    return jnp.cumsum(forget_each_token, axis=1).astype(jnp.float32)


def spiked(result, key, source, target, blocks, factor):
    def block_of(axis_at):
        return (jnp.arange(result.shape[axis_at]) // (result.shape[axis_at] // blocks)).reshape((-1,) + (1,) * (result.ndim - 1 - axis_at))

    one_side = jax.random.permutation(key, blocks)[block_of(target)]
    second = (block_of(target) + blocks // 2) % blocks
    return jnp.where((block_of(source) == one_side) | (block_of(source) == second), factor * result, result)


def levels(key, shape, cuts, smallest, high):
    def one(dim, blocks):
        draws = jax.random.uniform(jax.random.fold_in(jax.random.fold_in(key, 6), dim), (blocks,), jnp.float32, smallest / len(cuts), high / len(cuts))
        return jnp.repeat(jnp.exp(draws), shape[dim] // blocks).reshape((-1,) + (1,) * (len(shape) - dim - 1))

    level = one(*cuts[0])
    for cut in cuts[1:]:
        level = level * one(*cut)
    return level


def distinct(rng, rows, count, top, lift):
    ranking = jax.random.permutation(jax.random.fold_in(rng, 1), count)
    favour = ranking
    for power in range(3):
        favour = favour * favour // count
    favour = favour * lift // count
    chance = jax.random.randint(jax.random.fold_in(rng, 2), (rows, count), 0, 4096) + favour
    holders = jax.random.permutation(jax.random.fold_in(rng, 3), rows)[jnp.arange(count) % rows]
    chance = jnp.where(jnp.arange(rows)[:, None] == holders[None, :], 1 << 14, chance)
    merit = chance * count + jnp.arange(count)
    return lax.top_k(merit.astype(jnp.int32), top)[1].astype(jnp.int32)


def scatter_about(key, extent, spread, most, shards=(), kind=jnp.bfloat16):
    entries = jax.random.normal(key, extent, jnp.float32) * spread
    if len(shards) > 0:
        entries = levels(key, extent, shards, -0.22, 0.18) * entries
    return jnp.clip(entries, min=-most, max=most).astype(kind)


def noise_with(rng, shape, scale, limit, pieces, heavy, held_as=jnp.bfloat16):
    entries = scale * jax.random.normal(rng, shape, jnp.float32)
    if pieces:
        entries = entries * levels(rng, shape, pieces, -0.22, 0.18)
    return jnp.clip(spiked(entries, jax.random.fold_in(rng, 3), *heavy), -limit, limit).astype(held_as)


def setup_inputs(seed: int = 0, part: int = 0) -> dict:
    keys = jax.random.split(jax.random.key(seed), 23)
    part_keys = jax.random.split(jax.random.fold_in(keys[22], part), 23)
    tokens = noise_with(part_keys[0], (BATCH_LENGTH, D), 1.0, 6.0, ((1, 32),), (1, 0, 32, 2.75))
    w_query = scatter_about(keys[1], (D, ATT), D ** -0.5, 0.125, ((0, 32),))
    w_key = scatter_about(keys[2], (D, ATT), D ** -0.5, 0.125, ((0, 32),))
    w_value = scatter_about(keys[3], (D, ATT), D ** -0.5, 0.125, ((0, 32),))
    w_forget = scatter_about(keys[4], (D, QUERY_GROUPS), D ** -0.5, 0.125, ((0, 32),))
    forget_bias = jnp.clip(jax.random.uniform(keys[5], (QUERY_GROUPS,), jnp.float32, -1.0, 2.0), -1.0, 2.0)
    cache_keys = draw_cache_keys(jax.random.fold_in(jax.random.fold_in(keys[22], part), 71), part)
    cache_values = scatter_about(part_keys[7], (BATCH_LENGTH, STORED_PLACES, ATT), 1.0, 6.0, ((0, 32),))
    cache_gates = draw_cache_gates(jax.random.fold_in(jax.random.fold_in(keys[22], part), 71), part)
    lengths = draw_lengths(jax.random.fold_in(jax.random.fold_in(keys[22], part), 71), part)
    w_out = scatter_about(keys[10], (ATT, D), ATT ** -0.5, 0.1875, ((0, 32),))
    norm_gain = jnp.clip(1.0 + 0.18 * jax.random.normal(keys[11], (D,), jnp.float32), 0.099609375, 1.8984375).astype(jnp.bfloat16)
    w_router = scatter_about(keys[12], (D, EXPERTS), D ** -0.5, 0.125)
    routes = distinct(part_keys[13], BATCH_LENGTH, EXPERTS, TOPK, 4096)
    dense_gate = scatter_about(keys[14], (D,), (D // 4) ** -0.5, 0.25)
    dense_w_gate = scatter_about(keys[15], (D, DENSE_FF), D ** -0.5, 0.125, ((1, 32),))
    dense_w_up = scatter_about(keys[16], (D, DENSE_FF), D ** -0.5, 0.125, ((1, 32),))
    dense_w_down = noise_with(keys[17], (DENSE_FF, D), DENSE_FF ** -0.5, 0.125, ((0, 32),), (0, 1, 32, 2.75))
    expert_w_gate = scatter_about(keys[18], (D, EXPERTS * EXPERT_FF), D ** -0.5, 0.125, ((1, 32),))
    expert_w_up = scatter_about(keys[19], (D, EXPERTS * EXPERT_FF), D ** -0.5, 0.125, ((1, 32),))
    expert_w_down = noise_with(keys[20], (EXPERTS * EXPERT_FF, D), EXPERT_FF ** -0.5, 0.1875, ((0, 32),), (0, 1, 32, 2.75))
    final_gain = jnp.clip(1.0 + 0.18 * jax.random.normal(keys[21], (D,), jnp.float32), 0.099609375, 1.8984375).astype(jnp.bfloat16)
    return dict(tokens=tokens, w_query=w_query, w_key=w_key, w_value=w_value, w_forget=w_forget, forget_bias=forget_bias, cache_keys=cache_keys, cache_values=cache_values, cache_gates=cache_gates, lengths=lengths, w_out=w_out, norm_gain=norm_gain, w_router=w_router, routes=routes, dense_gate=dense_gate, dense_w_gate=dense_w_gate, dense_w_up=dense_w_up, dense_w_down=dense_w_down, expert_w_gate=expert_w_gate, expert_w_up=expert_w_up, expert_w_down=expert_w_down, final_gain=final_gain)


norm_eps = 1e-05
residual_scale = 8.0 ** 0.25

def norm_rows(values, weights):
    center = lax.optimization_barrier(jnp.mean(values, axis=-1, keepdims=True))
    second = lax.optimization_barrier(jnp.mean(values * values, axis=-1, keepdims=True))
    return (values - center) * lax.rsqrt(second - center * center + norm_eps) * weights.astype(jnp.float32)

def attend(query, new_key, new_value, forget_pre, forget_bias, cache_keys, cache_values, cache_gates, lengths):
    seqs_here, width = query.shape
    heads = cache_gates.shape[2]
    head_size = width // heads
    cache_len = cache_keys.shape[1]
    query = query.reshape(seqs_here, heads, head_size).astype(jnp.float32)
    new_key = new_key.reshape(seqs_here, heads, head_size).astype(jnp.float32)
    new_value = new_value.reshape(seqs_here, heads, head_size).astype(jnp.float32)
    keys_all = cache_keys.reshape(seqs_here, cache_len, heads, head_size).astype(jnp.float32)
    values_all = cache_values.reshape(seqs_here, cache_len, heads, head_size).astype(jnp.float32)
    log_gate = jax.nn.log_sigmoid(forget_pre + forget_bias[None, :])
    position = jnp.arange(cache_len, dtype=jnp.int32)
    is_last = (position[None, :] == (lengths - 1)[:, None]).astype(jnp.float32)
    last_gate = lax.optimization_barrier(jnp.sum(cache_gates * is_last[:, :, None], axis=1))
    bias = (last_gate + log_gate)[:, :, None] - jnp.transpose(cache_gates, (0, 2, 1))
    scale = head_size ** (-0.5)
    scores = jnp.einsum('shd,slhd->shl', query, keys_all) * scale + bias
    valid = (position[None, :] < lengths[:, None])[:, None, :]
    scores = jnp.where(valid, scores, -jnp.inf)
    own_score = lax.optimization_barrier(jnp.sum(query * new_key, axis=-1)) * scale
    top = jnp.maximum(lax.optimization_barrier(jnp.max(scores, axis=-1)), own_score)
    weights_cache = jnp.exp(scores - top[:, :, None])
    weight_own = jnp.exp(own_score - top)
    total = lax.optimization_barrier(jnp.sum(weights_cache, axis=-1)) + weight_own
    probs = (weights_cache / total[:, :, None]).astype(jnp.bfloat16)
    prob_own = (weight_own / total).astype(jnp.bfloat16)
    mixed = jnp.einsum('shl,slhd->shd', probs.astype(jnp.float32), values_all)
    mixed = mixed + prob_own.astype(jnp.float32)[:, :, None] * new_value
    return mixed.astype(jnp.bfloat16).reshape(seqs_here, width)

def reference(tokens, w_query, w_key, w_value, w_forget, forget_bias, cache_keys, cache_values, cache_gates, lengths, w_out, norm_gain, w_router, routes, dense_gate, dense_w_gate, dense_w_up, dense_w_down, expert_w_gate, expert_w_up, expert_w_down, final_gain):
    query = jnp.dot(tokens, w_query, preferred_element_type=jnp.float32).astype(jnp.bfloat16)
    new_key = jnp.dot(tokens, w_key, preferred_element_type=jnp.float32).astype(jnp.bfloat16)
    new_value = jnp.dot(tokens, w_value, preferred_element_type=jnp.float32).astype(jnp.bfloat16)
    forget_pre = jnp.dot(tokens, w_forget, preferred_element_type=jnp.float32)
    attn = attend(query, new_key, new_value, forget_pre, forget_bias, cache_keys, cache_values, cache_gates, lengths)
    mixed = residual_scale * tokens.astype(jnp.float32) + jnp.dot(attn, w_out, preferred_element_type=jnp.float32)
    normed = norm_rows(mixed, norm_gain).astype(jnp.bfloat16)
    logits = jnp.dot(normed, w_router, preferred_element_type=jnp.float32)
    expert_count = w_router.shape[1]
    picks = (routes[:, :, None] == jnp.arange(expert_count, dtype=jnp.int32)[None, None, :]).astype(jnp.float32)
    chosen = lax.optimization_barrier(jnp.sum(logits[:, None, :] * picks, axis=-1))
    route_weight = jax.nn.softmax(chosen, axis=-1)
    per_expert = lax.optimization_barrier(jnp.sum(route_weight[:, :, None] * picks, axis=1))
    expert_width = expert_w_gate.shape[1] // expert_count
    branch = jnp.zeros((tokens.shape[0], tokens.shape[1]), jnp.float32)
    for index in range(expert_count):
        low = index * expert_width
        gate_part = jnp.dot(normed, expert_w_gate[:, low:low + expert_width], preferred_element_type=jnp.float32)
        up_part = jnp.dot(normed, expert_w_up[:, low:low + expert_width], preferred_element_type=jnp.float32)
        hidden = (per_expert[:, index:index + 1] * jax.nn.silu(gate_part) * up_part).astype(jnp.bfloat16)
        branch = branch + jnp.dot(hidden, expert_w_down[low:low + expert_width], preferred_element_type=jnp.float32)
    dense_scale = jax.nn.sigmoid(jnp.dot(normed, dense_gate, preferred_element_type=jnp.float32))
    dense_gate_part = jnp.dot(normed, dense_w_gate, preferred_element_type=jnp.float32)
    dense_up_part = jnp.dot(normed, dense_w_up, preferred_element_type=jnp.float32)
    dense_hidden = (dense_scale[:, None] * jax.nn.silu(dense_gate_part) * dense_up_part).astype(jnp.bfloat16)
    branch = branch + jnp.dot(dense_hidden, dense_w_down, preferred_element_type=jnp.float32)
    final = residual_scale * normed.astype(jnp.float32) + branch
    return norm_rows(final, final_gain).astype(jnp.bfloat16)
```

```python
import functools

import jax
import jax.numpy as jnp
from jax import lax
from jax.experimental import pallas as pl
from jax.experimental.pallas import tpu as pltpu
from jax.sharding import PartitionSpec as P

norm_eps = 1e-05
residual_scale = 8.0**0.25
MESH = pl.DeviceIdType.MESH
F32 = jnp.float32
BF16 = jnp.bfloat16
LANES = 128
HIGH = lax.Precision.HIGHEST


def iota(shape, dim):
    return lax.broadcasted_iota(jnp.int32, shape, dim)


def dot(a, b):
    return jnp.dot(a, b, preferred_element_type=F32)


def dot_nt(a, b, precision=None):
    return lax.dot_general(
        a, b, (((1,), (1,)), ((), ())), precision=precision, preferred_element_type=F32
    )


def silu(v):
    return v / (1.0 + jnp.exp(-v))


def column_of(row, count):
    shape = (count, row.shape[1])
    hit = iota(shape, 0) == iota(shape, 1)
    return jnp.sum(jnp.where(hit, jnp.broadcast_to(row, shape), 0.0), axis=1, keepdims=True)


def layer_kernel(
    devices,
    lengths,
    tokens,
    w_query,
    w_key,
    w_value,
    w_forget,
    forget_bias,
    w_out,
    norm_gain,
    w_router,
    routes,
    dense_gate,
    final_gain,
    cache_keys,
    cache_values,
    cache_gates,
    expert_w_gate,
    expert_w_up,
    dense_w_gate,
    dense_w_up,
    expert_w_down,
    dense_w_down,
    out,
    keys_v,
    values_v,
    gates_v,
    eg_v,
    eu_v,
    dg_v,
    du_v,
    ed_v,
    dd_v,
    proj,
    proj_in,
    reduced,
    qkv,
    forget,
    forget_in,
    tok_own,
    tok_pair,
    wcol,
    attn_f,
    attn_own,
    attn_in,
    mixed_own,
    mixed_all,
    normed_v,
    branch_v,
    branch_in,
    fin_own,
    fin_pair,
    stat_own,
    stat_in,
    local_sem,
    send_sem,
    recv_sem,
    pair_sem,
):
    me = lax.axis_index("ep")
    seqs, feat = tokens.shape
    seqs_here, cache_len, width = cache_keys.shape
    heads = cache_gates.shape[2]
    head_size = width // heads
    model = norm_gain.shape[1]
    experts = w_router.shape[1]
    rows_f = forget_in.shape[1]
    rows_p = proj_in.shape[1]
    cols_p = proj_in.shape[2]
    members = devices // (seqs // rows_p)
    per_f = rows_f // seqs_here
    half = seqs // 2
    pair = me // 2
    side = me % 2
    partner = 2 * pair + 1 - side
    block = 2 * feat

    barrier = pltpu.get_barrier_semaphore()

    def greet(step, carry):
        pl.semaphore_signal(
            barrier, inc=1, device_id={"ep": (me + step) % devices}, device_id_type=MESH
        )
        return carry

    lax.fori_loop(1, devices, greet, 0)

    big = (
        (cache_gates, gates_v),
        (cache_keys, keys_v),
        (cache_values, values_v),
        (expert_w_gate, eg_v),
        (expert_w_up, eu_v),
        (dense_w_gate, dg_v),
        (dense_w_up, du_v),
        (expert_w_down, ed_v),
        (dense_w_down, dd_v),
    )
    loads = [
        pltpu.make_async_copy(src, dst, local_sem.at[i]) for i, (src, dst) in enumerate(big)
    ]
    for load in loads:
        load.start()

    def remote(phase, src, dst, dest, slot, origin):
        return pltpu.make_async_remote_copy(
            src_ref=src,
            dst_ref=dst,
            send_sem=send_sem.at[phase, slot],
            recv_sem=recv_sem.at[phase, origin],
            device_id={"ep": dest},
            device_id_type=MESH,
        )

    def each(count, mine, fn):
        def body(step, carry):
            fn((mine + step) % count)
            return carry

        lax.fori_loop(1, count, body, 0)

    x = tokens[...]
    proj[:, 0:width] = dot(x, w_query[...]).astype(BF16)
    proj[:, width : 2 * width] = dot(x, w_key[...]).astype(BF16)
    proj[:, 2 * width : 3 * width] = dot(x, w_value[...]).astype(BF16)
    forget[...] = jnp.zeros_like(forget)
    forget[:, 0:heads] = dot(x, w_forget[...])
    place = (iota((feat, block), 1) == iota((feat, block), 0) + side * feat).astype(BF16)
    tok_own[...] = dot(x, place).astype(BF16)

    pl.semaphore_wait(barrier, devices - 1)

    def proj_src(d):
        return proj.at[
            pl.ds(pl.multiple_of(rows_p * (d // members), rows_p), rows_p),
            pl.ds(pl.multiple_of(cols_p * (d % members), LANES), cols_p),
        ]

    def forget_src(d):
        return forget.at[pl.ds(pl.multiple_of(rows_f * (d // per_f), rows_f), rows_f)]

    def wout_src(d):
        return w_out.at[:, pl.ds(pl.multiple_of(block * (d // 2), LANES), block)]

    def copy_proj(d, origin):
        return remote(0, proj_src(d), proj_in.at[origin], d, d, origin)

    def copy_forget(d, origin):
        return remote(1, forget_src(d), forget_in.at[origin], d, d, origin)

    def copy_wout(d, origin):
        return remote(2, wout_src(d), wcol.at[origin], d, d, origin)

    each(devices, me, lambda d: copy_proj(d, me).start())
    each(devices, me, lambda d: copy_forget(d, me).start())
    each(devices, me, lambda d: copy_wout(d, me).start())
    tok_copy = pltpu.make_async_remote_copy(
        src_ref=tok_own,
        dst_ref=tok_pair,
        send_sem=pair_sem.at[0],
        recv_sem=pair_sem.at[1],
        device_id={"ep": partner},
        device_id_type=MESH,
    )
    tok_copy.start()

    proj_in[me] = proj[
        pl.ds(pl.multiple_of(rows_p * (me // members), rows_p), rows_p),
        pl.ds(pl.multiple_of(cols_p * (me % members), LANES), cols_p),
    ]
    forget_in[me] = forget[pl.ds(pl.multiple_of(rows_f * (me // per_f), rows_f), rows_f), :]
    wcol[me] = w_out[:, pl.ds(pl.multiple_of(block * pair, LANES), block)]

    loads[0].wait()
    eye = (iota((heads, heads), 0) == iota((heads, heads), 1)).astype(F32)
    position = iota((heads, cache_len), 1)
    gates_t = []
    for b in range(seqs_here):
        turned = dot_nt(eye, gates_v[b], HIGH)
        last = jnp.sum(
            jnp.where(position == lengths[b] - 1, turned, 0.0), axis=1, keepdims=True
        )
        gates_t.append(last - turned)

    each(devices, me, lambda d: copy_proj(d, d).wait_recv())
    total = proj_in[0].astype(F32)
    for s in range(1, devices):
        total = total + proj_in[s].astype(F32)
    reduced[...] = total.astype(BF16)

    group = me // members
    member = me % members

    def qkv_slot(m):
        return qkv.at[:, pl.ds(pl.multiple_of(cols_p * m, LANES), cols_p)]

    def copy_group(m, origin):
        return remote(3, reduced, qkv_slot(origin), group * members + m, m, origin)

    each(members, member, lambda m: copy_group(m, member).start())
    qkv[:, pl.ds(pl.multiple_of(cols_p * member, LANES), cols_p)] = total.astype(BF16)

    each(devices, me, lambda d: copy_forget(d, d).wait_recv())
    forget_sum = forget_in[0]
    for s in range(1, devices):
        forget_sum = forget_sum + forget_in[s]

    each(members, member, lambda m: copy_group(m, m).wait_recv())
    mine = qkv[...].astype(F32)
    scale = head_size ** (-0.5)
    diagonal = iota((heads, width), 1) // head_size == iota((heads, width), 0)
    loads[1].wait()
    loads[2].wait()
    for b in range(seqs_here):
        at_p = iota(mine.shape, 0) == seqs_here * member + b
        row = jnp.sum(jnp.where(at_p, mine, 0.0), axis=0, keepdims=True)
        at_f = iota(forget_sum.shape, 0) == seqs_here * (me % per_f) + b
        pre = jnp.sum(jnp.where(at_f, forget_sum, 0.0), axis=0, keepdims=True)
        pre = column_of(pre, heads) + column_of(forget_bias[...], heads)
        log_gate = jnp.minimum(pre, 0.0) - jnp.log(1.0 + jnp.exp(-jnp.abs(pre)))
        query = jnp.where(diagonal, row[:, 0:width], 0.0)
        own_score = jnp.sum(query * row[:, width : 2 * width], axis=1, keepdims=True) * scale
        scores = dot_nt(query.astype(BF16), keys_v[b]) * scale + (gates_t[b] + log_gate)
        scores = jnp.where(position < lengths[b], scores, -jnp.inf)
        top = jnp.maximum(jnp.max(scores, axis=1, keepdims=True), own_score)
        weights = jnp.exp(scores - top)
        own = jnp.exp(own_score - top)
        total_w = jnp.sum(weights, axis=1, keepdims=True) + own
        probs = (weights / total_w).astype(BF16)
        own = (own / total_w).astype(BF16).astype(F32)
        seen = dot(probs, values_v[b]) + own * row[:, 2 * width : 3 * width]
        attn_row = jnp.sum(jnp.where(diagonal, seen, 0.0), axis=0, keepdims=True)
        for j in range(width // LANES):
            at = b * (width // LANES) + j
            attn_f[at : at + 1, :] = attn_row[:, j * LANES : (j + 1) * LANES]
    attn_own[...] = attn_f[...].astype(BF16)

    def copy_attn(d, origin):
        return remote(4, attn_own, attn_in.at[origin], d, d, origin)

    each(devices, me, lambda d: copy_attn(d, me).start())
    attn_in[me] = attn_own[...]
    tok_copy.wait_recv()
    residual = residual_scale * (tok_own[...].astype(F32) + tok_pair[...].astype(F32))
    each(devices, me, lambda d: copy_wout(d, d).wait_recv())
    each(devices, me, lambda d: copy_attn(d, d).wait_recv())

    pieces = width // LANES
    attn_all = attn_in[...].reshape(seqs * pieces, LANES)
    w_cols = wcol[...].reshape(width, block)
    acc = jnp.zeros((seqs * pieces, block), F32)
    turn = iota((seqs * pieces, block), 0) % pieces
    for j in range(pieces):
        part = dot(attn_all, w_cols[j * LANES : (j + 1) * LANES, :])
        acc = jnp.where(turn == j, part, acc)
    mixed = residual + jnp.sum(acc.reshape(seqs, pieces, block), axis=1)
    mixed_own[...] = mixed.astype(BF16)

    def copy_mixed(k, origin):
        return remote(
            5,
            mixed_own,
            mixed_all.at[:, pl.ds(pl.multiple_of(block * origin, LANES), block)],
            2 * k + side,
            k,
            origin,
        )

    pairs = devices // 2
    each(pairs, pair, lambda k: copy_mixed(k, pair).start())
    mixed_all[:, pl.ds(pl.multiple_of(block * pair, LANES), block)] = mixed.astype(BF16)
    each(pairs, pair, lambda k: copy_mixed(k, k).wait_recv())

    mixed = mixed_all[...].astype(F32)
    center = jnp.mean(mixed, axis=1, keepdims=True)
    second = jnp.mean(mixed * mixed, axis=1, keepdims=True)
    normed = (
        (mixed - center)
        * lax.rsqrt(second - center * center + norm_eps)
        * norm_gain[...].astype(F32)
    ).astype(BF16)
    normed_v[...] = normed

    logits = dot(normed, w_router[...])
    first, other = routes[:, 0:1], routes[:, 1:2]
    shape = logits.shape
    chosen_a = jnp.sum(jnp.where(iota(shape, 1) == first, logits, 0.0), axis=1, keepdims=True)
    chosen_b = jnp.sum(jnp.where(iota(shape, 1) == other, logits, 0.0), axis=1, keepdims=True)
    top = jnp.maximum(chosen_a, chosen_b)
    exp_a, exp_b = jnp.exp(chosen_a - top), jnp.exp(chosen_b - top)
    expert = me // (devices // experts)
    share = (
        jnp.where(first == expert, exp_a, 0.0) + jnp.where(other == expert, exp_b, 0.0)
    ) / (exp_a + exp_b)
    dense_pre = jnp.sum(
        normed.astype(F32) * dense_gate[...].astype(F32), axis=1, keepdims=True
    )
    dense_scale = 1.0 / (1.0 + jnp.exp(-dense_pre))

    loads[3].wait()
    loads[4].wait()
    hidden_e = (share * silu(dot(normed, eg_v[...])) * dot(normed, eu_v[...])).astype(BF16)
    loads[5].wait()
    loads[6].wait()
    hidden_d = (dense_scale * silu(dot(normed, dg_v[...])) * dot(normed, du_v[...])).astype(BF16)
    loads[7].wait()
    loads[8].wait()
    branch_v[...] = (dot(hidden_e, ed_v[...]) + dot(hidden_d, dd_v[...])).astype(BF16)

    def branch_at(d):
        return (
            pl.ds(pl.multiple_of(half * (d % 2), half), half),
            pl.ds(pl.multiple_of(block * (d // 2), LANES), block),
        )

    def copy_branch(d, origin):
        return remote(6, branch_v.at[branch_at(d)], branch_in.at[origin], d, d, origin)

    each(devices, me, lambda d: copy_branch(d, me).start())
    branch_in[me] = branch_v[branch_at(me)]
    each(devices, me, lambda d: copy_branch(d, d).wait_recv())
    final = residual_scale * normed_v[branch_at(me)].astype(F32)
    for s in range(devices):
        final = final + branch_in[s].astype(F32)
    fin_own[...] = final
    fin_copy = pltpu.make_async_remote_copy(
        src_ref=fin_own,
        dst_ref=fin_pair,
        send_sem=pair_sem.at[2],
        recv_sem=pair_sem.at[3],
        device_id={"ep": partner},
        device_id_type=MESH,
    )
    fin_copy.start()
    ones = jnp.ones((stat_own.shape[0], block), F32)
    sums = dot_nt(ones, final, HIGH)
    squares = dot_nt(ones, final * final, HIGH)
    stat_own[...] = jnp.zeros_like(stat_own)
    stat_own[:, 0:half] = jnp.where(iota(sums.shape, 0) == 0, sums, squares)

    def copy_stat(d, origin):
        return remote(7, stat_own, stat_in.at[origin], d, d, origin)

    each(devices, me, lambda d: copy_stat(d, me).start())
    stat_in[me] = stat_own[...]
    fin_copy.wait_recv()
    each(devices, me, lambda d: copy_stat(d, d).wait_recv())

    other_final = fin_pair[...]
    gain = final_gain[...].astype(F32)
    for p in range(2):
        stat = stat_in[p]
        for s in range(p + 2, devices, 2):
            stat = stat + stat_in[s]
        center = column_of(stat[0:1, :], half) / model
        second = column_of(stat[1:2, :], half) / model
        value = jnp.where(side == p, final, other_final)
        unit = (value - center) * lax.rsqrt(second - center * center + norm_eps)
        unit = jnp.where(side == 0, unit, pltpu.roll(unit, feat, 1))
        out[p * half : (p + 1) * half, :] = (unit[:, 0:feat] * gain).astype(BF16)

    each(devices, me, lambda d: copy_proj(d, me).wait_send())
    each(devices, me, lambda d: copy_forget(d, me).wait_send())
    each(devices, me, lambda d: copy_wout(d, me).wait_send())
    each(members, member, lambda m: copy_group(m, member).wait_send())
    each(devices, me, lambda d: copy_attn(d, me).wait_send())
    each(pairs, pair, lambda k: copy_mixed(k, pair).wait_send())
    each(devices, me, lambda d: copy_branch(d, me).wait_send())
    each(devices, me, lambda d: copy_stat(d, me).wait_send())
    tok_copy.wait_send()
    fin_copy.wait_send()


def shards(
    devices,
    tokens,
    w_query,
    w_key,
    w_value,
    w_forget,
    forget_bias,
    cache_keys,
    cache_values,
    cache_gates,
    lengths,
    w_out,
    norm_gain,
    w_router,
    routes,
    dense_gate,
    dense_w_gate,
    dense_w_up,
    dense_w_down,
    expert_w_gate,
    expert_w_up,
    expert_w_down,
    final_gain,
):
    seqs, feat = tokens.shape
    seqs_here, cache_len, width = cache_keys.shape
    model = norm_gain.shape[0]
    rows_p, rows_f = 16, 8
    members = devices // (seqs // rows_p)
    cols_p = 3 * width // members
    block = 2 * feat
    half = seqs // 2
    pieces = width // LANES
    vmem = pl.BlockSpec(memory_space=pltpu.VMEM)
    hbm = pl.BlockSpec(memory_space=pl.ANY)
    big = (
        cache_keys,
        cache_values,
        cache_gates,
        expert_w_gate,
        expert_w_up,
        dense_w_gate,
        dense_w_up,
        expert_w_down,
        dense_w_down,
    )
    return pl.pallas_call(
        functools.partial(layer_kernel, devices),
        out_shape=jax.ShapeDtypeStruct((seqs, feat), BF16),
        in_specs=[pl.BlockSpec(memory_space=pltpu.SMEM)] + [vmem] * 12 + [hbm] * len(big),
        out_specs=vmem,
        scratch_shapes=[pltpu.VMEM(a.shape, a.dtype) for a in big]
        + [
            pltpu.VMEM((seqs, 3 * width), BF16),
            pltpu.VMEM((devices, rows_p, cols_p), BF16),
            pltpu.VMEM((rows_p, cols_p), BF16),
            pltpu.VMEM((rows_p, 3 * width), BF16),
            pltpu.VMEM((seqs, LANES), F32),
            pltpu.VMEM((devices, rows_f, LANES), F32),
            pltpu.VMEM((seqs, block), BF16),
            pltpu.VMEM((seqs, block), BF16),
            pltpu.VMEM((devices, width // devices, block), BF16),
            pltpu.VMEM((seqs_here * pieces, LANES), F32),
            pltpu.VMEM((seqs_here * pieces, LANES), BF16),
            pltpu.VMEM((devices, seqs_here * pieces, LANES), BF16),
            pltpu.VMEM((seqs, block), BF16),
            pltpu.VMEM((seqs, model), BF16),
            pltpu.VMEM((seqs, model), BF16),
            pltpu.VMEM((seqs, model), BF16),
            pltpu.VMEM((devices, half, block), BF16),
            pltpu.VMEM((half, block), F32),
            pltpu.VMEM((half, block), F32),
            pltpu.VMEM((8, LANES), F32),
            pltpu.VMEM((devices, 8, LANES), F32),
            pltpu.SemaphoreType.DMA((len(big),)),
            pltpu.SemaphoreType.DMA((8, devices)),
            pltpu.SemaphoreType.DMA((8, devices)),
            pltpu.SemaphoreType.DMA((4,)),
        ],
        compiler_params=pltpu.CompilerParams(
            collective_id=0, has_side_effects=True, vmem_limit_bytes=60 * 1024 * 1024
        ),
    )(
        lengths,
        tokens,
        w_query,
        w_key,
        w_value,
        w_forget,
        forget_bias[None, :],
        w_out,
        norm_gain[None, :],
        w_router,
        routes,
        dense_gate[None, :],
        final_gain[None, :],
        *big,
    )


def solution(mesh):
    placed = (
        P("grp", "ep"),
        P("ep", None),
        P("ep", None),
        P("ep", None),
        P("ep", None),
        P(),
        P(("grp", "ep"), None, None),
        P(("grp", "ep"), None, None),
        P(("grp", "ep"), None, None),
        P(("grp", "ep")),
        P("ep", None),
        P(),
        P(),
        P("grp", None),
        P(),
        P(None, "ep"),
        P(None, "ep"),
        P("ep", None),
        P(None, "ep"),
        P(None, "ep"),
        P("ep", None),
        P("ep"),
    )
    return jax.shard_map(
        functools.partial(shards, mesh.shape["ep"]),
        mesh=mesh,
        in_specs=placed,
        out_specs=P("grp", "ep"),
        check_vma=False,
    )
```

```python
import functools

import jax
import jax.numpy as jnp
from jax import lax
from jax.experimental import pallas as pl
from jax.experimental.pallas import tpu as pltpu
from jax.sharding import PartitionSpec as P

norm_eps = 1e-05
residual_scale = 8.0**0.25
MESH = pl.DeviceIdType.MESH
F32 = jnp.float32
BF16 = jnp.bfloat16
LANES = 128
HIGH = lax.Precision.HIGHEST


def iota(shape, dim):
    return lax.broadcasted_iota(jnp.int32, shape, dim)


def dot(a, b):
    return jnp.dot(a, b, preferred_element_type=F32)


def dot_nt(a, b, precision=None):
    return lax.dot_general(
        a, b, (((1,), (1,)), ((), ())), precision=precision, preferred_element_type=F32
    )


def silu(v):
    return v / (1.0 + jnp.exp(-v))


def column_of(row, count, start=0):
    shape = (count, row.shape[1])
    hit = iota(shape, 0) + start == iota(shape, 1)
    return jnp.sum(jnp.where(hit, jnp.broadcast_to(row, shape), 0.0), axis=1, keepdims=True)


def row_of(tile):
    tile = tile.astype(F32)
    return jnp.concatenate([tile[i : i + 1, :] for i in range(tile.shape[0])], axis=1)


def layer_kernel(
    devices,
    lengths,
    tokens,
    w_query,
    w_key,
    w_value,
    w_forget,
    forget_bias,
    w_out,
    norm_gain,
    w_router,
    routes,
    dense_gate,
    final_gain,
    cache_keys,
    cache_values,
    cache_gates,
    expert_w_gate,
    expert_w_up,
    dense_w_gate,
    dense_w_up,
    expert_w_down,
    dense_w_down,
    out,
    keys_v,
    values_v,
    gates_v,
    eg_v,
    eu_v,
    dg_v,
    du_v,
    ed_v,
    dd_v,
    proj,
    proj_pair,
    proj_sum,
    proj_in,
    reduced,
    qkv,
    forget,
    forget_in,
    forget_quad,
    tok_own,
    tok_pair,
    wcol,
    attn_f,
    attn_own,
    attn_in,
    mixed_own,
    mixed_all,
    normed_v,
    branch_v,
    branch_pair,
    branch_sum,
    branch_in,
    fin_own,
    fin_pair,
    stat_own,
    stat_in,
    local_sem,
    send_sem,
    recv_sem,
    pair_sem,
):
    me = lax.axis_index("ep")
    seqs, feat = tokens.shape
    seqs_here, cache_len, width = cache_keys.shape
    heads = cache_gates.shape[1]
    head_size = width // heads
    model = mixed_all.shape[1]
    experts = w_router.shape[0]
    rows_f = forget_in.shape[1]
    rows_p = proj_in.shape[1]
    cols_p = proj_in.shape[2]
    members = devices // (seqs // rows_p)
    per_f = rows_f // seqs_here
    half = seqs // 2
    pair = me // 2
    side = me % 2
    partner = 2 * pair + 1 - side
    block = 2 * feat
    pairs = devices // 2
    side_w = proj_pair.shape[1]
    groups_f = seqs // rows_f
    group = me // members
    member = me % members
    group_f = me // per_f
    member_f = me % per_f

    barrier = pltpu.get_barrier_semaphore()

    def greet(step, carry):
        pl.semaphore_signal(
            barrier, inc=1, device_id={"ep": (me + step) % devices}, device_id_type=MESH
        )
        return carry

    lax.fori_loop(1, devices, greet, 0)

    big = (
        (cache_gates, gates_v),
        (cache_keys, keys_v),
        (cache_values, values_v),
        (expert_w_gate, eg_v),
        (expert_w_up, eu_v),
        (dense_w_gate, dg_v),
        (dense_w_up, du_v),
        (expert_w_down, ed_v),
        (dense_w_down, dd_v),
    )
    loads = [
        pltpu.make_async_copy(src, dst, local_sem.at[i]) for i, (src, dst) in enumerate(big)
    ]
    for load in loads:
        load.start()

    def remote(phase, src, dst, dest, slot, origin):
        return pltpu.make_async_remote_copy(
            src_ref=src,
            dst_ref=dst,
            send_sem=send_sem.at[phase, slot],
            recv_sem=recv_sem.at[phase, origin],
            device_id={"ep": dest},
            device_id_type=MESH,
        )

    def each(count, mine, fn):
        def body(step, carry):
            fn((mine + step) % count)
            return carry

        lax.fori_loop(1, count, body, 0)

    x = tokens[...]
    proj[:, 0:width] = dot(x, w_query[...]).astype(BF16)
    proj[:, width : 2 * width] = dot(x, w_key[...]).astype(BF16)
    proj[:, 2 * width : 3 * width] = dot(x, w_value[...]).astype(BF16)
    forget[...] = jnp.zeros_like(forget)
    forget[:, 0:heads] = dot_nt(x, w_forget[...])
    place = (iota((feat, block), 1) == iota((feat, block), 0) + side * feat).astype(BF16)
    tok_own[...] = dot(x, place).astype(BF16)

    pl.semaphore_wait(barrier, devices - 1)

    def pair_copy(i, src, dst):
        return pltpu.make_async_remote_copy(
            src_ref=src,
            dst_ref=dst,
            send_sem=pair_sem.at[2 * i],
            recv_sem=pair_sem.at[2 * i + 1],
            device_id={"ep": partner},
            device_id_type=MESH,
        )

    def side_cols(at):
        return pl.ds(pl.multiple_of(side_w * at, LANES), side_w)

    def block_cols(k):
        return pl.ds(pl.multiple_of(block * k, LANES), block)

    def piece(m):
        return (m % 2) * (members // 2) + m // 2

    def proj_at(k):
        d = 2 * k + side
        return (
            pl.ds(pl.multiple_of(rows_p * (d // members), rows_p), rows_p),
            pl.ds(pl.multiple_of(cols_p * ((d % members) // 2), LANES), cols_p),
        )

    def forget_at(g):
        return pl.ds(pl.multiple_of(rows_f * g, rows_f), rows_f)

    def copy_proj(k, origin):
        return remote(0, proj_sum.at[proj_at(k)], proj_in.at[origin], 2 * k + side, k, origin)

    def copy_forget(g, origin):
        return remote(
            1, forget.at[forget_at(g)], forget_in.at[origin], per_f * g + member_f, g, origin
        )

    def copy_wout(k, origin):
        return remote(
            2, w_out.at[:, block_cols(k)], wcol.at[origin, side], 2 * k + side, k, origin
        )

    proj_copy = pair_copy(2, proj.at[:, side_cols(1 - side)], proj_pair)
    proj_copy.start()
    each(groups_f, group_f, lambda g: copy_forget(g, group_f).start())
    tok_copy = pair_copy(0, tok_own, tok_pair)
    tok_copy.start()
    forget_in[group_f] = forget[forget_at(group_f), :]
    proj_copy.wait_recv()
    proj_sum[...] = (
        proj[:, side_cols(side)].astype(F32) + proj_pair[...].astype(F32)
    ).astype(BF16)
    each(pairs, pair, lambda k: copy_proj(k, pair).start())
    proj_in[pair] = proj_sum[proj_at(pair)]
    wcol[pair, side] = w_out[:, block_cols(pair)]

    each(groups_f, group_f, lambda g: copy_forget(g, g).wait_recv())
    forget_sum = forget_in[0]
    for g in range(1, groups_f):
        forget_sum = forget_sum + forget_in[g]
    forget_quad[member_f] = forget_sum

    def copy_quad(m, origin):
        return remote(
            8, forget_quad.at[member_f], forget_quad.at[origin], per_f * group_f + m, m, origin
        )

    each(per_f, member_f, lambda m: copy_quad(m, member_f).start())

    loads[0].wait()
    position = iota((heads, cache_len), 1)
    gates_t = []
    for b in range(seqs_here):
        turned = gates_v[b]
        last = jnp.sum(
            jnp.where(position == lengths[b] - 1, turned, 0.0), axis=1, keepdims=True
        )
        gates_t.append(last - turned)

    each(pairs, pair, lambda k: copy_proj(k, k).wait_recv())
    total = proj_in[0].astype(F32)
    for s in range(1, pairs):
        total = total + proj_in[s].astype(F32)
    reduced[...] = total.astype(BF16)

    def qkv_cols(m):
        return pl.ds(pl.multiple_of(cols_p * piece(m), LANES), cols_p)

    def copy_group(m, origin):
        return remote(
            3, reduced, qkv.at[:, qkv_cols(origin)], group * members + m, m, origin
        )

    each(members, member, lambda m: copy_group(m, member).start())
    each(pairs, pair, lambda k: copy_wout(k, pair).start())
    qkv[:, qkv_cols(member)] = total.astype(BF16)

    each(per_f, member_f, lambda m: copy_quad(m, m).wait_recv())
    forget_sum = forget_quad[0]
    for m in range(1, per_f):
        forget_sum = forget_sum + forget_quad[m]

    each(members, member, lambda m: copy_group(m, m).wait_recv())
    mine = qkv[...].astype(F32)
    scale = head_size ** (-0.5)
    diagonal = iota((heads, width), 1) // head_size == iota((heads, width), 0)
    loads[1].wait()
    loads[2].wait()
    for b in range(seqs_here):
        at_p = iota(mine.shape, 0) == seqs_here * member + b
        row = jnp.sum(jnp.where(at_p, mine, 0.0), axis=0, keepdims=True)
        at_f = iota(forget_sum.shape, 0) == seqs_here * member_f + b
        pre = jnp.sum(jnp.where(at_f, forget_sum, 0.0), axis=0, keepdims=True)
        pre = column_of(pre, heads) + column_of(forget_bias[...], heads)
        log_gate = jnp.minimum(pre, 0.0) - jnp.log(1.0 + jnp.exp(-jnp.abs(pre)))
        query = jnp.where(diagonal, row[:, 0:width], 0.0)
        own_score = jnp.sum(query * row[:, width : 2 * width], axis=1, keepdims=True) * scale
        scores = dot_nt(query.astype(BF16), keys_v[b]) * scale + (gates_t[b] + log_gate)
        scores = jnp.where(position < lengths[b], scores, -jnp.inf)
        top = jnp.maximum(jnp.max(scores, axis=1, keepdims=True), own_score)
        weights = jnp.exp(scores - top)
        own = jnp.exp(own_score - top)
        total_w = jnp.sum(weights, axis=1, keepdims=True) + own
        probs = (weights / total_w).astype(BF16)
        own = (own / total_w).astype(BF16).astype(F32)
        seen = dot(probs, values_v[b]) + own * row[:, 2 * width : 3 * width]
        attn_row = jnp.sum(jnp.where(diagonal, seen, 0.0), axis=0, keepdims=True)
        for j in range(width // LANES):
            at = b * (width // LANES) + j
            attn_f[at : at + 1, :] = attn_row[:, j * LANES : (j + 1) * LANES]
    attn_own[...] = attn_f[...].astype(BF16)

    def copy_attn(d, origin):
        return remote(4, attn_own, attn_in.at[origin], d, d, origin)

    each(devices, me, lambda d: copy_attn(d, me).start())
    attn_in[me] = attn_own[...]
    tok_copy.wait_recv()
    residual = residual_scale * (tok_own[...].astype(F32) + tok_pair[...].astype(F32))
    each(pairs, pair, lambda k: copy_wout(k, k).wait_recv())
    wout_copy = pair_copy(3, wcol.at[:, side], wcol.at[:, side])
    wout_copy.start()
    wout_copy.wait_recv()
    each(devices, me, lambda d: copy_attn(d, d).wait_recv())

    pieces = width // LANES
    attn_all = attn_in[...].reshape(seqs * pieces, LANES)
    w_cols = wcol[...].reshape(width, block)
    acc = jnp.zeros((seqs * pieces, block), F32)
    turn = iota((seqs * pieces, block), 0) % pieces
    for j in range(pieces):
        part = dot(attn_all, w_cols[j * LANES : (j + 1) * LANES, :])
        acc = jnp.where(turn == j, part, acc)
    mixed = residual + jnp.sum(acc.reshape(seqs, pieces, block), axis=1)
    mixed_own[...] = mixed.astype(BF16)

    def copy_mixed(k, origin):
        return remote(
            5,
            mixed_own,
            mixed_all.at[:, block_cols(origin)],
            2 * k + side,
            k,
            origin,
        )

    each(pairs, pair, lambda k: copy_mixed(k, pair).start())
    mixed_all[:, block_cols(pair)] = mixed.astype(BF16)
    each(pairs, pair, lambda k: copy_mixed(k, k).wait_recv())

    mixed = mixed_all[...].astype(F32)
    center = jnp.mean(mixed, axis=1, keepdims=True)
    second = jnp.mean(mixed * mixed, axis=1, keepdims=True)
    normed = (
        (mixed - center)
        * lax.rsqrt(second - center * center + norm_eps)
        * row_of(norm_gain[...])
    ).astype(BF16)
    normed_v[...] = normed

    logits = dot_nt(normed, w_router[...])
    names = routes[...].astype(F32)
    first = column_of(names[0:1, :], seqs).astype(jnp.int32)
    other = column_of(names[1:2, :], seqs).astype(jnp.int32)
    shape = logits.shape
    chosen_a = jnp.sum(jnp.where(iota(shape, 1) == first, logits, 0.0), axis=1, keepdims=True)
    chosen_b = jnp.sum(jnp.where(iota(shape, 1) == other, logits, 0.0), axis=1, keepdims=True)
    top = jnp.maximum(chosen_a, chosen_b)
    exp_a, exp_b = jnp.exp(chosen_a - top), jnp.exp(chosen_b - top)
    expert = me // (devices // experts)
    share = (
        jnp.where(first == expert, exp_a, 0.0) + jnp.where(other == expert, exp_b, 0.0)
    ) / (exp_a + exp_b)
    dense_pre = jnp.sum(
        normed.astype(F32) * row_of(dense_gate[...]), axis=1, keepdims=True
    )
    dense_scale = 1.0 / (1.0 + jnp.exp(-dense_pre))

    loads[3].wait()
    loads[4].wait()
    hidden_e = (share * silu(dot(normed, eg_v[...])) * dot(normed, eu_v[...])).astype(BF16)
    loads[5].wait()
    loads[6].wait()
    hidden_d = (dense_scale * silu(dot(normed, dg_v[...])) * dot(normed, du_v[...])).astype(BF16)
    loads[7].wait()
    loads[8].wait()
    branch_v[...] = (dot(hidden_e, ed_v[...]) + dot(hidden_d, dd_v[...])).astype(BF16)

    def half_rows(at):
        return pl.ds(pl.multiple_of(half * at, half), half)

    branch_copy = pair_copy(4, branch_v.at[half_rows(1 - side)], branch_pair)
    branch_copy.start()
    final = residual_scale * normed_v[half_rows(side), block_cols(pair)].astype(F32)
    branch_copy.wait_recv()
    branch_sum[...] = (
        branch_v[half_rows(side), :].astype(F32) + branch_pair[...].astype(F32)
    ).astype(BF16)

    def copy_branch(k, origin):
        return remote(
            6, branch_sum.at[:, block_cols(k)], branch_in.at[origin], 2 * k + side, k, origin
        )

    each(pairs, pair, lambda k: copy_branch(k, pair).start())
    branch_in[pair] = branch_sum[:, block_cols(pair)]
    each(pairs, pair, lambda k: copy_branch(k, k).wait_recv())
    for s in range(pairs):
        final = final + branch_in[s].astype(F32)
    fin_own[...] = final
    fin_copy = pair_copy(1, fin_own, fin_pair)
    fin_copy.start()
    ones = jnp.ones((8, block), F32)
    sums = dot_nt(ones, final, HIGH)
    squares = dot_nt(ones, final * final, HIGH)
    stat_own[...] = jnp.zeros_like(stat_own)
    stat_own[:, 0:half] = sums[0:1, :]
    stat_own[:, half : 2 * half] = squares[0:1, :]

    def copy_stat(d, origin):
        return remote(7, stat_own, stat_in.at[origin], d, d, origin)

    each(devices, me, lambda d: copy_stat(d, me).start())
    stat_in[me] = stat_own[...]
    fin_copy.wait_recv()
    each(devices, me, lambda d: copy_stat(d, d).wait_recv())

    other_final = fin_pair[...]
    gain = final_gain[...].astype(F32)
    for p in range(2):
        stat = stat_in[p]
        for s in range(p + 2, devices, 2):
            stat = stat + stat_in[s]
        center = column_of(stat, half) / model
        second = column_of(stat, half, half) / model
        value = jnp.where(side == p, final, other_final)
        unit = (value - center) * lax.rsqrt(second - center * center + norm_eps)
        unit = jnp.where(side == 0, unit, pltpu.roll(unit, feat, 1))
        out[p * half : (p + 1) * half, :] = (unit[:, 0:feat] * gain).astype(BF16)

    each(groups_f, group_f, lambda g: copy_forget(g, group_f).wait_send())
    each(per_f, member_f, lambda m: copy_quad(m, member_f).wait_send())
    each(members, member, lambda m: copy_group(m, member).wait_send())
    each(devices, me, lambda d: copy_attn(d, me).wait_send())
    each(devices, me, lambda d: copy_stat(d, me).wait_send())
    for copy in (copy_proj, copy_wout, copy_mixed, copy_branch):
        each(pairs, pair, lambda k: copy(k, pair).wait_send())
    for copy in (proj_copy, tok_copy, wout_copy, branch_copy, fin_copy):
        copy.wait_send()


def shards(
    devices,
    tokens,
    w_query,
    w_key,
    w_value,
    w_forget,
    forget_bias,
    cache_keys,
    cache_values,
    cache_gates,
    lengths,
    w_out,
    norm_gain,
    w_router,
    routes,
    dense_gate,
    dense_w_gate,
    dense_w_up,
    dense_w_down,
    expert_w_gate,
    expert_w_up,
    expert_w_down,
    final_gain,
):
    seqs, feat = tokens.shape
    seqs_here, cache_len, width = cache_keys.shape
    model = norm_gain.shape[0]
    rows_p, rows_f = 16, 8
    members = devices // (seqs // rows_p)
    cols_p = 3 * width // members
    block = 2 * feat
    half = seqs // 2
    pieces = width // LANES
    pairs = devices // 2
    per_f = rows_f // seqs_here
    vmem = pl.BlockSpec(memory_space=pltpu.VMEM)
    hbm = pl.BlockSpec(memory_space=pl.ANY)
    big = (
        cache_keys,
        cache_values,
        jnp.transpose(cache_gates, (0, 2, 1)),
        expert_w_gate,
        expert_w_up,
        dense_w_gate,
        dense_w_up,
        expert_w_down,
        dense_w_down,
    )
    return pl.pallas_call(
        functools.partial(layer_kernel, devices),
        out_shape=jax.ShapeDtypeStruct((seqs, feat), BF16),
        in_specs=[pl.BlockSpec(memory_space=pltpu.SMEM)] + [vmem] * 12 + [hbm] * len(big),
        out_specs=vmem,
        scratch_shapes=[pltpu.VMEM(a.shape, a.dtype) for a in big]
        + [
            pltpu.VMEM((seqs, 3 * width), BF16),
            pltpu.VMEM((seqs, 3 * width // 2), BF16),
            pltpu.VMEM((seqs, 3 * width // 2), BF16),
            pltpu.VMEM((pairs, rows_p, cols_p), BF16),
            pltpu.VMEM((rows_p, cols_p), BF16),
            pltpu.VMEM((rows_p, 3 * width), BF16),
            pltpu.VMEM((seqs, LANES), F32),
            pltpu.VMEM((seqs // rows_f, rows_f, LANES), F32),
            pltpu.VMEM((per_f, rows_f, LANES), F32),
            pltpu.VMEM((seqs, block), BF16),
            pltpu.VMEM((seqs, block), BF16),
            pltpu.VMEM((pairs, 2, width // devices, block), BF16),
            pltpu.VMEM((seqs_here * pieces, LANES), F32),
            pltpu.VMEM((seqs_here * pieces, LANES), BF16),
            pltpu.VMEM((devices, seqs_here * pieces, LANES), BF16),
            pltpu.VMEM((seqs, block), BF16),
            pltpu.VMEM((seqs, model), BF16),
            pltpu.VMEM((seqs, model), BF16),
            pltpu.VMEM((seqs, model), BF16),
            pltpu.VMEM((half, model), BF16),
            pltpu.VMEM((half, model), BF16),
            pltpu.VMEM((pairs, half, block), BF16),
            pltpu.VMEM((half, block), F32),
            pltpu.VMEM((half, block), F32),
            pltpu.VMEM((1, LANES), F32),
            pltpu.VMEM((devices, 1, LANES), F32),
            pltpu.SemaphoreType.DMA((len(big),)),
            pltpu.SemaphoreType.DMA((9, devices)),
            pltpu.SemaphoreType.DMA((9, devices)),
            pltpu.SemaphoreType.DMA((10,)),
        ],
        compiler_params=pltpu.CompilerParams(
            collective_id=0, has_side_effects=True, vmem_limit_bytes=60 * 1024 * 1024
        ),
    )(
        lengths,
        tokens,
        w_query,
        w_key,
        w_value,
        w_forget.T,
        forget_bias[None, :],
        w_out,
        norm_gain.reshape(-1, LANES),
        w_router.T,
        routes.T,
        dense_gate.reshape(-1, LANES),
        final_gain[None, :],
        *big,
    )


def solution(mesh):
    placed = (
        P("grp", "ep"),
        P("ep", None),
        P("ep", None),
        P("ep", None),
        P("ep", None),
        P(),
        P(("grp", "ep"), None, None),
        P(("grp", "ep"), None, None),
        P(("grp", "ep"), None, None),
        P(("grp", "ep")),
        P("ep", None),
        P(),
        P(),
        P("grp", None),
        P(),
        P(None, "ep"),
        P(None, "ep"),
        P("ep", None),
        P(None, "ep"),
        P(None, "ep"),
        P("ep", None),
        P("ep"),
    )
    return jax.shard_map(
        functools.partial(shards, mesh.shape["ep"]),
        mesh=mesh,
        in_specs=placed,
        out_specs=P("grp", "ep"),
        check_vma=False,
    )
```

```python
import functools

import jax
import jax.numpy as jnp
from jax import lax
from jax.experimental import pallas as pl
from jax.experimental.pallas import tpu as pltpu
from jax.sharding import PartitionSpec as P

norm_eps = 1e-05
residual_scale = 8.0**0.25
MESH = pl.DeviceIdType.MESH
F32 = jnp.float32
BF16 = jnp.bfloat16
LANES = 128
HIGH = lax.Precision.HIGHEST


def iota(shape, dim):
    return lax.broadcasted_iota(jnp.int32, shape, dim)


def dot(a, b):
    return jnp.dot(a, b, preferred_element_type=F32)


def dot_nt(a, b, precision=None):
    return lax.dot_general(
        a, b, (((1,), (1,)), ((), ())), precision=precision, preferred_element_type=F32
    )


def silu(v):
    return v / (1.0 + jnp.exp(-v))


def column_of(row, count, start=0):
    shape = (count, row.shape[1])
    hit = iota(shape, 0) + start == iota(shape, 1)
    return jnp.sum(jnp.where(hit, jnp.broadcast_to(row, shape), 0.0), axis=1, keepdims=True)


def row_of(tile):
    tile = tile.astype(F32)
    return jnp.concatenate([tile[i : i + 1, :] for i in range(tile.shape[0])], axis=1)


def layer_kernel(
    devices,
    lengths,
    tokens,
    w_query,
    w_key,
    w_value,
    w_forget,
    forget_bias,
    w_out,
    norm_gain,
    w_router,
    routes,
    dense_gate,
    final_gain,
    cache_keys,
    cache_values,
    cache_gates,
    expert_w_gate,
    expert_w_up,
    dense_w_gate,
    dense_w_up,
    expert_w_down,
    dense_w_down,
    out,
    keys_v,
    values_v,
    gates_v,
    eg_v,
    eu_v,
    dg_v,
    du_v,
    ed_v,
    dd_v,
    proj,
    proj_pair,
    proj_sum,
    proj_in,
    reduced,
    qkv,
    forget,
    forget_in,
    forget_quad,
    tok_own,
    tok_pair,
    wcol,
    attn_f,
    attn_own,
    attn_in,
    mixed_own,
    mixed_all,
    normed_v,
    branch_v,
    branch_pair,
    branch_sum,
    branch_in,
    fin_own,
    fin_pair,
    stat_own,
    stat_in,
    local_sem,
    send_sem,
    recv_sem,
    pair_sem,
):
    me = lax.axis_index("ep")
    seqs, feat = tokens.shape
    seqs_here, cache_len, width = cache_keys.shape
    heads = cache_gates.shape[1]
    head_size = width // heads
    model = mixed_all.shape[1]
    experts = w_router.shape[0]
    rows_f = forget_in.shape[1]
    rows_p = proj_in.shape[1]
    cols_p = proj_in.shape[2]
    members = devices // (seqs // rows_p)
    per_f = rows_f // seqs_here
    half = seqs // 2
    pair = me // 2
    side = me % 2
    partner = 2 * pair + 1 - side
    block = 2 * feat
    pairs = devices // 2
    side_w = proj_pair.shape[1]
    groups_f = seqs // rows_f
    group = me // members
    member = me % members
    group_f = me // per_f
    member_f = me % per_f

    barrier = pltpu.get_barrier_semaphore()

    def greet(step, carry):
        pl.semaphore_signal(
            barrier, inc=1, device_id={"ep": (me + step) % devices}, device_id_type=MESH
        )
        return carry

    lax.fori_loop(1, devices, greet, 0)

    big = (
        (cache_gates, gates_v),
        (cache_keys, keys_v),
        (cache_values, values_v),
        (expert_w_gate, eg_v),
        (expert_w_up, eu_v),
        (dense_w_gate, dg_v),
        (dense_w_up, du_v),
        (expert_w_down, ed_v),
        (dense_w_down, dd_v),
    )
    loads = [
        pltpu.make_async_copy(src, dst, local_sem.at[i]) for i, (src, dst) in enumerate(big)
    ]
    for load in loads:
        load.start()

    def remote(phase, src, dst, dest, slot, origin):
        return pltpu.make_async_remote_copy(
            src_ref=src,
            dst_ref=dst,
            send_sem=send_sem.at[phase, slot],
            recv_sem=recv_sem.at[phase, origin],
            device_id={"ep": dest},
            device_id_type=MESH,
        )

    def each(count, mine, fn):
        def body(step, carry):
            fn((mine + step) % count)
            return carry

        lax.fori_loop(1, count, body, 0)

    x = tokens[...]
    proj[:, 0:width] = dot(x, w_query[...]).astype(BF16)
    proj[:, width : 2 * width] = dot(x, w_key[...]).astype(BF16)
    proj[:, 2 * width : 3 * width] = dot(x, w_value[...]).astype(BF16)
    forget[...] = jnp.zeros_like(forget)
    forget[:, 0:heads] = dot_nt(x, w_forget[...])
    place = (iota((feat, block), 1) == iota((feat, block), 0) + side * feat).astype(BF16)
    tok_own[...] = dot(x, place).astype(BF16)

    pl.semaphore_wait(barrier, devices - 1)

    def pair_copy(i, src, dst):
        return pltpu.make_async_remote_copy(
            src_ref=src,
            dst_ref=dst,
            send_sem=pair_sem.at[2 * i],
            recv_sem=pair_sem.at[2 * i + 1],
            device_id={"ep": partner},
            device_id_type=MESH,
        )

    def side_cols(at):
        return pl.ds(pl.multiple_of(side_w * at, LANES), side_w)

    def block_cols(k):
        return pl.ds(pl.multiple_of(block * k, LANES), block)

    def piece(m):
        return (m % 2) * (members // 2) + m // 2

    def proj_at(k):
        d = 2 * k + side
        return (
            pl.ds(pl.multiple_of(rows_p * (d // members), rows_p), rows_p),
            pl.ds(pl.multiple_of(cols_p * ((d % members) // 2), LANES), cols_p),
        )

    def forget_at(g):
        return pl.ds(pl.multiple_of(rows_f * g, rows_f), rows_f)

    def copy_proj(k, origin):
        return remote(0, proj_sum.at[proj_at(k)], proj_in.at[origin], 2 * k + side, k, origin)

    def copy_forget(g, origin):
        return remote(
            1, forget.at[forget_at(g)], forget_in.at[origin], per_f * g + member_f, g, origin
        )

    def copy_wout(k, origin):
        return remote(
            2, w_out.at[:, block_cols(k)], wcol.at[origin, side], 2 * k + side, k, origin
        )

    proj_copy = pair_copy(2, proj.at[:, side_cols(1 - side)], proj_pair)
    proj_copy.start()
    each(groups_f, group_f, lambda g: copy_forget(g, group_f).start())
    tok_copy = pair_copy(0, tok_own, tok_pair)
    tok_copy.start()
    forget_in[group_f] = forget[forget_at(group_f), :]
    proj_copy.wait_recv()
    proj_sum[...] = (
        proj[:, side_cols(side)].astype(F32) + proj_pair[...].astype(F32)
    ).astype(BF16)
    each(pairs, pair, lambda k: copy_proj(k, pair).start())
    proj_in[pair] = proj_sum[proj_at(pair)]
    wcol[pair, side] = w_out[:, block_cols(pair)]

    each(groups_f, group_f, lambda g: copy_forget(g, g).wait_recv())
    forget_sum = forget_in[0]
    for g in range(1, groups_f):
        forget_sum = forget_sum + forget_in[g]
    forget_quad[member_f] = forget_sum

    def copy_quad(m, origin):
        return remote(
            8, forget_quad.at[member_f], forget_quad.at[origin], per_f * group_f + m, m, origin
        )

    each(per_f, member_f, lambda m: copy_quad(m, member_f).start())

    loads[0].wait()
    position = iota((heads, cache_len), 1)
    gates_t = []
    for b in range(seqs_here):
        turned = gates_v[b]
        last = jnp.sum(
            jnp.where(position == lengths[b] - 1, turned, 0.0), axis=1, keepdims=True
        )
        gates_t.append(last - turned)

    each(pairs, pair, lambda k: copy_proj(k, k).wait_recv())
    total = proj_in[0].astype(F32)
    for s in range(1, pairs):
        total = total + proj_in[s].astype(F32)
    reduced[...] = total.astype(BF16)

    def qkv_cols(m):
        return pl.ds(pl.multiple_of(cols_p * piece(m), LANES), cols_p)

    def copy_group(m, origin):
        return remote(
            3, reduced, qkv.at[:, qkv_cols(origin)], group * members + m, m, origin
        )

    each(members, member, lambda m: copy_group(m, member).start())
    each(pairs, pair, lambda k: copy_wout(k, pair).start())
    qkv[:, qkv_cols(member)] = total.astype(BF16)

    each(per_f, member_f, lambda m: copy_quad(m, m).wait_recv())
    forget_sum = forget_quad[0]
    for m in range(1, per_f):
        forget_sum = forget_sum + forget_quad[m]

    each(members, member, lambda m: copy_group(m, m).wait_recv())
    mine = qkv[...].astype(F32)
    scale = head_size ** (-0.5)
    diagonal = iota((heads, width), 1) // head_size == iota((heads, width), 0)
    loads[1].wait()
    loads[2].wait()
    for b in range(seqs_here):
        at_p = iota(mine.shape, 0) == seqs_here * member + b
        row = jnp.sum(jnp.where(at_p, mine, 0.0), axis=0, keepdims=True)
        at_f = iota(forget_sum.shape, 0) == seqs_here * member_f + b
        pre = jnp.sum(jnp.where(at_f, forget_sum, 0.0), axis=0, keepdims=True)
        pre = column_of(pre, heads) + column_of(forget_bias[...], heads)
        log_gate = jnp.minimum(pre, 0.0) - jnp.log(1.0 + jnp.exp(-jnp.abs(pre)))
        query = jnp.where(diagonal, row[:, 0:width], 0.0)
        own_score = jnp.sum(query * row[:, width : 2 * width], axis=1, keepdims=True) * scale
        scores = dot_nt(query.astype(BF16), keys_v[b]) * scale + (gates_t[b] + log_gate)
        scores = jnp.where(position < lengths[b], scores, -jnp.inf)
        top = jnp.maximum(jnp.max(scores, axis=1, keepdims=True), own_score)
        weights = jnp.exp(scores - top)
        own = jnp.exp(own_score - top)
        total_w = jnp.sum(weights, axis=1, keepdims=True) + own
        probs = (weights / total_w).astype(BF16)
        own = (own / total_w).astype(BF16).astype(F32)
        seen = dot(probs, values_v[b]) + own * row[:, 2 * width : 3 * width]
        attn_row = jnp.sum(jnp.where(diagonal, seen, 0.0), axis=0, keepdims=True)
        for j in range(width // LANES):
            at = b * (width // LANES) + j
            attn_f[at : at + 1, :] = attn_row[:, j * LANES : (j + 1) * LANES]
    attn_own[...] = attn_f[...].astype(BF16)

    share_of = devices // 2
    rank_half = me // share_of
    rank_slot = me % share_of

    def half_rows(at):
        return pl.ds(pl.multiple_of(half * at, half), half)

    def copy_attn(k, origin):
        return remote(4, attn_own, attn_in.at[origin], 2 * k + rank_half, k, origin)

    def attn_sends(fn):
        def body(step, carry):
            k = (pair + step) % pairs

            @pl.when(2 * k + rank_half != me)
            def _():
                fn(copy_attn(k, rank_slot))

            return carry

        lax.fori_loop(0, pairs, body, 0)

    def attn_arrivals():
        def body(j, carry):
            @pl.when(share_of * side + j != me)
            def _():
                copy_attn(j, j).wait_recv()

            return carry

        lax.fori_loop(0, share_of, body, 0)

    attn_sends(lambda copy: copy.start())

    @pl.when(rank_half == side)
    def _():
        attn_in[rank_slot] = attn_own[...]

    tok_copy.wait_recv()
    residual = residual_scale * (
        tok_own[half_rows(side), :].astype(F32) + tok_pair[half_rows(side), :].astype(F32)
    )
    each(pairs, pair, lambda k: copy_wout(k, k).wait_recv())
    wout_copy = pair_copy(3, wcol.at[:, side], wcol.at[:, side])
    wout_copy.start()
    wout_copy.wait_recv()
    attn_arrivals()

    pieces = width // LANES
    attn_all = attn_in[...].reshape(half * pieces, LANES)
    w_cols = wcol[...].reshape(width, block)
    acc = jnp.zeros((half * pieces, block), F32)
    turn = iota((half * pieces, block), 0) % pieces
    for j in range(pieces):
        part = dot(attn_all, w_cols[j * LANES : (j + 1) * LANES, :])
        acc = jnp.where(turn == j, part, acc)
    mixed = residual + jnp.sum(acc.reshape(half, pieces, block), axis=1)
    mixed_own[...] = mixed.astype(BF16)

    def copy_mixed(k, origin):
        return remote(
            5,
            mixed_own,
            mixed_all.at[:, block_cols(origin)],
            2 * k + side,
            k,
            origin,
        )

    each(pairs, pair, lambda k: copy_mixed(k, pair).start())
    mixed_all[:, block_cols(pair)] = mixed.astype(BF16)
    each(pairs, pair, lambda k: copy_mixed(k, k).wait_recv())

    mixed = mixed_all[...].astype(F32)
    center = jnp.mean(mixed, axis=1, keepdims=True)
    second = jnp.mean(mixed * mixed, axis=1, keepdims=True)
    normed = (
        (mixed - center)
        * lax.rsqrt(second - center * center + norm_eps)
        * row_of(norm_gain[...])
    ).astype(BF16)
    normed_v[half_rows(side), :] = normed
    normed_copy = pair_copy(
        5, normed_v.at[half_rows(side)], normed_v.at[half_rows(side)]
    )
    normed_copy.start()
    normed_copy.wait_recv()
    normed = normed_v[...]

    logits = dot_nt(normed, w_router[...])
    names = routes[...].astype(F32)
    first = column_of(names[0:1, :], seqs).astype(jnp.int32)
    other = column_of(names[1:2, :], seqs).astype(jnp.int32)
    shape = logits.shape
    chosen_a = jnp.sum(jnp.where(iota(shape, 1) == first, logits, 0.0), axis=1, keepdims=True)
    chosen_b = jnp.sum(jnp.where(iota(shape, 1) == other, logits, 0.0), axis=1, keepdims=True)
    top = jnp.maximum(chosen_a, chosen_b)
    exp_a, exp_b = jnp.exp(chosen_a - top), jnp.exp(chosen_b - top)
    expert = me // (devices // experts)
    share = (
        jnp.where(first == expert, exp_a, 0.0) + jnp.where(other == expert, exp_b, 0.0)
    ) / (exp_a + exp_b)
    dense_pre = jnp.sum(
        normed.astype(F32) * row_of(dense_gate[...]), axis=1, keepdims=True
    )
    dense_scale = 1.0 / (1.0 + jnp.exp(-dense_pre))

    loads[3].wait()
    loads[4].wait()
    hidden_e = (share * silu(dot(normed, eg_v[...])) * dot(normed, eu_v[...])).astype(BF16)
    loads[5].wait()
    loads[6].wait()
    hidden_d = (dense_scale * silu(dot(normed, dg_v[...])) * dot(normed, du_v[...])).astype(BF16)
    loads[7].wait()
    loads[8].wait()
    branch_v[...] = (dot(hidden_e, ed_v[...]) + dot(hidden_d, dd_v[...])).astype(BF16)

    branch_copy = pair_copy(4, branch_v.at[half_rows(1 - side)], branch_pair)
    branch_copy.start()
    final = residual_scale * normed_v[half_rows(side), block_cols(pair)].astype(F32)
    branch_copy.wait_recv()
    branch_sum[...] = (
        branch_v[half_rows(side), :].astype(F32) + branch_pair[...].astype(F32)
    ).astype(BF16)

    def copy_branch(k, origin):
        return remote(
            6, branch_sum.at[:, block_cols(k)], branch_in.at[origin], 2 * k + side, k, origin
        )

    each(pairs, pair, lambda k: copy_branch(k, pair).start())
    branch_in[pair] = branch_sum[:, block_cols(pair)]
    each(pairs, pair, lambda k: copy_branch(k, k).wait_recv())
    for s in range(pairs):
        final = final + branch_in[s].astype(F32)
    fin_own[...] = final
    fin_copy = pair_copy(1, fin_own, fin_pair)
    fin_copy.start()
    ones = jnp.ones((8, block), F32)
    sums = dot_nt(ones, final, HIGH)
    squares = dot_nt(ones, final * final, HIGH)
    stat_own[...] = jnp.zeros_like(stat_own)
    stat_own[:, 0:half] = sums[0:1, :]
    stat_own[:, half : 2 * half] = squares[0:1, :]

    def copy_stat(d, origin):
        return remote(7, stat_own, stat_in.at[origin], d, d, origin)

    each(devices, me, lambda d: copy_stat(d, me).start())
    stat_in[me] = stat_own[...]
    fin_copy.wait_recv()
    each(devices, me, lambda d: copy_stat(d, d).wait_recv())

    other_final = fin_pair[...]
    gain = final_gain[...].astype(F32)
    for p in range(2):
        stat = stat_in[p]
        for s in range(p + 2, devices, 2):
            stat = stat + stat_in[s]
        center = column_of(stat, half) / model
        second = column_of(stat, half, half) / model
        value = jnp.where(side == p, final, other_final)
        unit = (value - center) * lax.rsqrt(second - center * center + norm_eps)
        unit = jnp.where(side == 0, unit, pltpu.roll(unit, feat, 1))
        out[p * half : (p + 1) * half, :] = (unit[:, 0:feat] * gain).astype(BF16)

    each(groups_f, group_f, lambda g: copy_forget(g, group_f).wait_send())
    each(per_f, member_f, lambda m: copy_quad(m, member_f).wait_send())
    each(members, member, lambda m: copy_group(m, member).wait_send())
    attn_sends(lambda copy: copy.wait_send())
    each(devices, me, lambda d: copy_stat(d, me).wait_send())
    for copy in (copy_proj, copy_wout, copy_mixed, copy_branch):
        each(pairs, pair, lambda k: copy(k, pair).wait_send())
    for copy in (proj_copy, tok_copy, wout_copy, normed_copy, branch_copy, fin_copy):
        copy.wait_send()


def shards(
    devices,
    tokens,
    w_query,
    w_key,
    w_value,
    w_forget,
    forget_bias,
    cache_keys,
    cache_values,
    cache_gates,
    lengths,
    w_out,
    norm_gain,
    w_router,
    routes,
    dense_gate,
    dense_w_gate,
    dense_w_up,
    dense_w_down,
    expert_w_gate,
    expert_w_up,
    expert_w_down,
    final_gain,
):
    seqs, feat = tokens.shape
    seqs_here, cache_len, width = cache_keys.shape
    model = norm_gain.shape[0]
    rows_p, rows_f = 16, 8
    members = devices // (seqs // rows_p)
    cols_p = 3 * width // members
    block = 2 * feat
    half = seqs // 2
    pieces = width // LANES
    pairs = devices // 2
    per_f = rows_f // seqs_here
    vmem = pl.BlockSpec(memory_space=pltpu.VMEM)
    hbm = pl.BlockSpec(memory_space=pl.ANY)
    big = (
        cache_keys,
        cache_values,
        jnp.transpose(cache_gates, (0, 2, 1)),
        expert_w_gate,
        expert_w_up,
        dense_w_gate,
        dense_w_up,
        expert_w_down,
        dense_w_down,
    )
    return pl.pallas_call(
        functools.partial(layer_kernel, devices),
        out_shape=jax.ShapeDtypeStruct((seqs, feat), BF16),
        in_specs=[pl.BlockSpec(memory_space=pltpu.SMEM)] + [vmem] * 12 + [hbm] * len(big),
        out_specs=vmem,
        scratch_shapes=[pltpu.VMEM(a.shape, a.dtype) for a in big]
        + [
            pltpu.VMEM((seqs, 3 * width), BF16),
            pltpu.VMEM((seqs, 3 * width // 2), BF16),
            pltpu.VMEM((seqs, 3 * width // 2), BF16),
            pltpu.VMEM((pairs, rows_p, cols_p), BF16),
            pltpu.VMEM((rows_p, cols_p), BF16),
            pltpu.VMEM((rows_p, 3 * width), BF16),
            pltpu.VMEM((seqs, LANES), F32),
            pltpu.VMEM((seqs // rows_f, rows_f, LANES), F32),
            pltpu.VMEM((per_f, rows_f, LANES), F32),
            pltpu.VMEM((seqs, block), BF16),
            pltpu.VMEM((seqs, block), BF16),
            pltpu.VMEM((pairs, 2, width // devices, block), BF16),
            pltpu.VMEM((seqs_here * pieces, LANES), F32),
            pltpu.VMEM((seqs_here * pieces, LANES), BF16),
            pltpu.VMEM((pairs, seqs_here * pieces, LANES), BF16),
            pltpu.VMEM((half, block), BF16),
            pltpu.VMEM((half, model), BF16),
            pltpu.VMEM((seqs, model), BF16),
            pltpu.VMEM((seqs, model), BF16),
            pltpu.VMEM((half, model), BF16),
            pltpu.VMEM((half, model), BF16),
            pltpu.VMEM((pairs, half, block), BF16),
            pltpu.VMEM((half, block), F32),
            pltpu.VMEM((half, block), F32),
            pltpu.VMEM((1, LANES), F32),
            pltpu.VMEM((devices, 1, LANES), F32),
            pltpu.SemaphoreType.DMA((len(big),)),
            pltpu.SemaphoreType.DMA((9, devices)),
            pltpu.SemaphoreType.DMA((9, devices)),
            pltpu.SemaphoreType.DMA((12,)),
        ],
        compiler_params=pltpu.CompilerParams(
            collective_id=0, has_side_effects=True, vmem_limit_bytes=60 * 1024 * 1024
        ),
    )(
        lengths,
        tokens,
        w_query,
        w_key,
        w_value,
        w_forget.T,
        forget_bias[None, :],
        w_out,
        norm_gain.reshape(-1, LANES),
        w_router.T,
        routes.T,
        dense_gate.reshape(-1, LANES),
        final_gain[None, :],
        *big,
    )


def solution(mesh):
    placed = (
        P("grp", "ep"),
        P("ep", None),
        P("ep", None),
        P("ep", None),
        P("ep", None),
        P(),
        P(("grp", "ep"), None, None),
        P(("grp", "ep"), None, None),
        P(("grp", "ep"), None, None),
        P(("grp", "ep")),
        P("ep", None),
        P(),
        P(),
        P("grp", None),
        P(),
        P(None, "ep"),
        P(None, "ep"),
        P("ep", None),
        P(None, "ep"),
        P(None, "ep"),
        P("ep", None),
        P("ep"),
    )
    return jax.shard_map(
        functools.partial(shards, mesh.shape["ep"]),
        mesh=mesh,
        in_specs=placed,
        out_specs=P("grp", "ep"),
        check_vma=False,
    )
```
